512 devices in a mesh: grp: 2 (over y), sp: 64 (over z, core), tp: 4 (over x).
Axes of the slice: x: 4, y: 2, z: 32, core: 2. Of those that a mesh axis runs over, the one named last changes fastest.
The devices are a block of a 4x8x32 slice.
Arguments:
- tokens: bfloat16 [65536, 2048], P(('grp', 'sp')), parts along dimension 0, may hold values from -6 to 6
- gate_in: bfloat16 [2, 2048, 512], P(None, 'sp', 'tp'), may hold values from -0.125 to 0.125
- gate_conv: bfloat16 [2, 2048, 512], P(None, 'sp', 'tp'), may hold values from -0.125 to 0.125
- value_in: bfloat16 [2, 2048, 512], P(None, 'sp', 'tp'), may hold values from -0.125 to 0.125
- out_weight: bfloat16 [2, 512, 2048], P(None, None, 'sp'), may hold values from -0.25 to 0.25
- conv_taps: float32 [2, 3, 512], replicated, may hold values from -7 to 7
- pre_gain: float32 [2, 2048], replicated, may hold values from 0.1 to 1.9
- mix_gain: float32 [2, 512], replicated, may hold values from 0.1 to 1.9
- post_gain: float32 [2, 2048], replicated, may hold values from 0.1 to 1.9
Outputs:
- result: bfloat16 [65536, 2048], P(('grp', 'sp', 'tp')), parts along dimension 0
The draws below stay inside these ranges and needn't reach their ends.
There are 2 independent parts, one for each index of `grp`. The reference program is written for one: setup_inputs(seed, part) draws one part's arguments, and reference() takes and returns one part's arrays. A program takes and returns all parts, laid end to end along the dimension named above; an argument that names none is the same for every part. Nothing has to cross between parts.
All inputs are finite; a program needn't handle non-finite values.
Results may differ from the reference program's by a relative error of at most 0.011.
Values may be sent and summed in bfloat16 or wider, within the bound.
No kernel may reach another device: no remote copies, remote signals or barrier semaphores. Data moves between devices by JAX's collectives and lax.ppermute only.
A program may use at most 64 MiB of HBM per device.

```python
import math
import jax
import jax.numpy as jnp
from jax import lax

D = 2048
S = 512
TAPS = 3
LAYERS = 2
TOKENS = 32768
TP_CH = 128


def draw_conv_taps(key, part):
    first_key, second_key = jax.random.split(jax.random.fold_in(key, 11))
    blocks = S // TP_CH
    orders = jax.vmap(lambda one_key: jax.random.permutation(one_key, blocks))(jax.random.split(first_key, LAYERS))
    ladder = 0.3 * jnp.power(10.0, orders.astype(jnp.float32) / max(blocks - 1, 1))
    raw_taps = jnp.clip(jax.random.normal(second_key, (LAYERS, TAPS, S), jnp.float32), -4.0, 4.0)
    scales = jnp.repeat(ladder, TP_CH, axis=1)
    return raw_taps * scales[:, None, :] / math.sqrt(TAPS)


def shard_levels(key, shape, shards, smallest, top_value):
    level = 1.0
    for dim, shards_of in shards:
        heights = jax.random.uniform(jax.random.fold_in(jax.random.fold_in(key, 6), dim), (shards_of,), jnp.float32, smallest / len(shards), top_value / len(shards))
        level = level * jnp.repeat(jnp.exp(heights), shape[dim] // shards_of).reshape((-1,) + (1,) * (len(shape) - 1 - dim))
    return level


def scatter_about(own_key, extent, scale, limit, cuts=(), dtype=jnp.bfloat16):
    loudness = shard_levels(own_key, extent, cuts, -0.22, 0.18) if cuts else 1.0
    array = jax.random.normal(own_key, extent, jnp.float32) * scale * loudness
    return jnp.minimum(jnp.maximum(array, -limit), limit).astype(dtype)


def setup_inputs(seed: int = 0, part: int = 0) -> dict:
    splits = jax.random.split(jax.random.key(seed), 10)
    own_keys = jax.random.split(jax.random.fold_in(splits[9], part), 10)
    return {
        "tokens": scatter_about(own_keys[0], (TOKENS, D), 1.0, 6.0, ((0, 64),)),
        "gate_in": scatter_about(splits[1], (LAYERS, D, S), D ** -0.5, 0.125, ((1, 64), (2, 4))),
        "gate_conv": scatter_about(splits[2], (LAYERS, D, S), D ** -0.5, 0.125, ((1, 64), (2, 4))),
        "value_in": scatter_about(splits[3], (LAYERS, D, S), D ** -0.5, 0.125, ((1, 64), (2, 4))),
        "out_weight": scatter_about(splits[4], (LAYERS, S, D), S ** -0.5, 0.25, ((2, 64),)),
        "conv_taps": draw_conv_taps(jax.random.fold_in(splits[9], 71), part),
        "pre_gain": jnp.clip(1.0 + 0.18 * jax.random.normal(splits[6], (LAYERS, D), jnp.float32), 0.1, 1.9),
        "mix_gain": jnp.clip(1.0 + 0.18 * jax.random.normal(splits[7], (LAYERS, S), jnp.float32), 0.1, 1.9),
        "post_gain": jnp.clip(1.0 + 0.18 * jax.random.normal(splits[8], (LAYERS, D), jnp.float32), 0.1, 1.9),
    }


EPS = 1e-06

def rms_norm(values, gain):
    return values * lax.rsqrt(lax.optimization_barrier(jnp.mean(values * values, axis=-1, keepdims=True)) + EPS) * gain

def stored(values):
    return lax.optimization_barrier(values.astype(jnp.bfloat16))

def reference(tokens, gate_in, gate_conv, value_in, out_weight, conv_taps, pre_gain, mix_gain, post_gain):
    stream = tokens.astype(jnp.float32)
    for layer_index in range(LAYERS):
        normed = stored(rms_norm(stream, pre_gain[layer_index]))
        outer = stored(jnp.dot(normed, gate_in[layer_index], preferred_element_type=jnp.float32))
        inner = stored(jnp.dot(normed, gate_conv[layer_index], preferred_element_type=jnp.float32))
        values = stored(jnp.dot(normed, value_in[layer_index], preferred_element_type=jnp.float32))
        gated = stored(inner.astype(jnp.float32) * values.astype(jnp.float32))
        padded = jnp.concatenate([jnp.zeros((TAPS - 1, S), jnp.bfloat16), gated], axis=0)
        filtered = jnp.zeros((TOKENS, S), jnp.float32)
        for tap_index in range(TAPS):
            filtered = filtered + conv_taps[layer_index, tap_index] * padded[tap_index:tap_index + TOKENS].astype(jnp.float32)
        mixed_raw = stored(outer.astype(jnp.float32) * filtered)
        mixed = stored(rms_norm(mixed_raw.astype(jnp.float32), mix_gain[layer_index]))
        branch = stored(jnp.dot(mixed, out_weight[layer_index], preferred_element_type=jnp.float32))
        stream = stream + rms_norm(branch.astype(jnp.float32), post_gain[layer_index])
    return stream.astype(jnp.bfloat16)
```

```python
import jax
import jax.numpy as jnp
from jax import lax
from jax.sharding import PartitionSpec as P

EPS = 1e-06
GATE_SCALE = 2.0**18
OUT_SCALE = 2.0**17


def passed_along(x, axis, by):
    length = lax.axis_size(axis)
    pairs = [(i, i + by) for i in range(length) if 0 <= i + by < length]
    return lax.ppermute(x, axis, pairs)


def rms_norm(values, gain):
    return values * lax.rsqrt(jnp.mean(values * values, axis=-1, keepdims=True) + EPS) * gain


def stored(values):
    return lax.optimization_barrier(values.astype(jnp.bfloat16))


def sent(values, scale):
    return (values.astype(jnp.float32) * scale).astype(jnp.float16)


def received(values, scale):
    return stored(values.astype(jnp.float32) * (1.0 / scale))


def per_device(
    tokens, gate_in, gate_conv, value_in, out_weight, conv_taps, pre_gain, mix_gain, post_gain
):
    layer_count = gate_in.shape[0]
    channel_count = gate_in.shape[2]
    whole_count = out_weight.shape[1]
    tap_count = conv_taps.shape[1]
    row_count = tokens.shape[0]
    tp_size = lax.axis_size("tp")
    tp_index = lax.axis_index("tp")
    row_share = row_count // tp_size
    pieces = []
    for layer_index in range(layer_count):
        for w in (gate_in, gate_conv, value_in):
            pieces.append(sent(w[layer_index], GATE_SCALE))
        pieces.append(sent(out_weight[layer_index].T, OUT_SCALE))
    packed = jnp.concatenate(pieces, axis=1)
    whole = lax.all_gather(packed, "sp", axis=0, tiled=True)
    stream = tokens.astype(jnp.float32)
    start = 0
    for layer_index in range(layer_count):
        is_last = layer_index == layer_count - 1
        gates = received(whole[:, start : start + 3 * channel_count], GATE_SCALE)
        start += 3 * channel_count
        out_whole = received(whole[:, start : start + whole_count], OUT_SCALE)
        start += whole_count
        normed = stored(rms_norm(stream, pre_gain[layer_index]))
        mixers = stored(jnp.dot(normed, gates, preferred_element_type=jnp.float32))
        outer = mixers[:, :channel_count]
        inner = mixers[:, channel_count : 2 * channel_count]
        values = mixers[:, 2 * channel_count :]
        gated = stored(inner.astype(jnp.float32) * values.astype(jnp.float32))
        before = passed_along(gated[row_count - (tap_count - 1) :], "sp", 1)
        padded = jnp.concatenate([before, gated], axis=0)
        taps_here = lax.dynamic_slice_in_dim(
            conv_taps[layer_index], tp_index * channel_count, channel_count, 1
        )
        filtered = jnp.zeros((row_count, channel_count), jnp.float32)
        for tap_index in range(tap_count):
            filtered = filtered + taps_here[tap_index] * padded[
                tap_index : tap_index + row_count
            ].astype(jnp.float32)
        mixed_raw = stored(outer.astype(jnp.float32) * filtered)
        if is_last:
            arrived = lax.all_to_all(mixed_raw, "tp", split_axis=0, concat_axis=1, tiled=True)
            residual = lax.dynamic_slice_in_dim(stream, tp_index * row_share, row_share, 0)
        else:
            arrived = lax.all_gather(mixed_raw, "tp", axis=1, tiled=True)
            residual = stream
        mixed = stored(rms_norm(arrived.astype(jnp.float32), mix_gain[layer_index]))
        branch = stored(
            lax.dot_general(
                mixed, out_whole, (((1,), (1,)), ((), ())), preferred_element_type=jnp.float32
            )
        )
        stream = residual + rms_norm(branch.astype(jnp.float32), post_gain[layer_index])
    return stream.astype(jnp.bfloat16)


def solution(mesh):
    placed = (
        P(("grp", "sp"), None),
        P(None, "sp", "tp"),
        P(None, "sp", "tp"),
        P(None, "sp", "tp"),
        P(None, None, "sp"),
        P(),
        P(),
        P(),
        P(),
    )
    return jax.shard_map(
        per_device,
        mesh=mesh,
        in_specs=placed,
        out_specs=P(("grp", "sp", "tp"), None),
        check_vma=False,
    )
```

```python
import jax
import jax.numpy as jnp
from jax import lax
from jax.experimental import pallas as pl
from jax.experimental.pallas import tpu as pltpu
from jax.sharding import PartitionSpec as P

EPS = 1e-06
GATE_SCALE = 2.0**18
OUT_SCALE = 2.0**17
HALO = 16
PAD = 8
BLOCK = 128
PARTS = 4

VMEM_LIMIT = 24 * 1024 * 1024


def scale_of(values, count):
    return lax.rsqrt(jnp.sum(values * values, axis=-1, keepdims=True) * (1.0 / count) + EPS)


def pack_kernel(gate_in, gate_conv, value_in, out_turned, tail, packed, tail_out):
    layers, _, channels = gate_in.shape
    whole = out_turned.shape[2]
    start = 0
    for layer in range(layers):
        for w in (gate_in, gate_conv, value_in):
            scaled = w[layer].astype(jnp.float32) * GATE_SCALE
            packed[:, start : start + channels] = scaled.astype(jnp.bfloat16)
            start += channels
        scaled = out_turned[layer].astype(jnp.float32) * OUT_SCALE
        packed[:, start : start + whole] = scaled.astype(jnp.bfloat16)
        start += whole
    tail_out[...] = tail[...]


def pack(tokens, gate_in, gate_conv, value_in, out_turned):
    rows = gate_in.shape[1]
    columns = gate_in.shape[0] * (3 * gate_in.shape[2] + out_turned.shape[2])
    count, width = tokens.shape
    return pl.pallas_call(
        pack_kernel,
        grid=(1,),
        in_specs=[
            pl.BlockSpec(gate_in.shape, lambda i: (0, 0, 0)),
            pl.BlockSpec(gate_in.shape, lambda i: (0, 0, 0)),
            pl.BlockSpec(gate_in.shape, lambda i: (0, 0, 0)),
            pl.BlockSpec(out_turned.shape, lambda i: (0, 0, 0)),
            pl.BlockSpec((HALO, width), lambda i: (count // HALO - 1, 0)),
        ],
        out_specs=[
            pl.BlockSpec((rows, columns), lambda i: (0, 0)),
            pl.BlockSpec((HALO, width), lambda i: (0, 0)),
        ],
        out_shape=[
            jax.ShapeDtypeStruct((rows, columns), jnp.bfloat16),
            jax.ShapeDtypeStruct((HALO, width), jnp.bfloat16),
        ],
        name="pack",
    )(gate_in, gate_conv, value_in, out_turned, tokens)


def in_blocks(rows):
    return [(0, HALO)] + [(HALO + start, BLOCK) for start in range(0, rows, BLOCK)]


def mix(normed, gates, taps, layer, tp_index, gated_rows, raw_of):
    rows = normed.shape[0]
    tap_count = taps.shape[1]
    channels = gates.shape[1] // 3
    mine = pl.ds(pl.multiple_of(tp_index * channels, channels), channels)
    mixers = jnp.dot(normed[...], gates[...], preferred_element_type=jnp.float32)
    mixers = mixers.astype(jnp.bfloat16).astype(jnp.float32)
    gated = mixers[:, channels : 2 * channels] * mixers[:, 2 * channels :]
    gated_rows[0:PAD, :] = jnp.zeros((PAD, channels), jnp.float32)
    gated_rows[PAD:, :] = gated.astype(jnp.bfloat16).astype(jnp.float32)
    filtered = None
    for tap in range(tap_count):
        at = PAD - (tap_count - 1) + tap
        term = taps[layer, tap : tap + 1, mine] * gated_rows[at : at + rows, :]
        filtered = term if filtered is None else filtered + term
    raw_of((mixers[:, :channels] * filtered).astype(jnp.bfloat16))


def first_kernel(
    tp_index, tokens, halo, gates, taps, pre_gain, raw, normed, gated_rows
):
    row_count, width = tokens.shape
    for first, count in in_blocks(row_count):
        rows = halo[...] if first == 0 else tokens[first - HALO : first - HALO + count, :]
        stream = rows.astype(jnp.float32)
        scale = scale_of(stream, width)
        normed[first : first + count, :] = (stream * scale * pre_gain[0:1, :]).astype(jnp.bfloat16)

    def store(values):
        for t in range(raw.shape[0]):
            raw[t] = values

    mix(normed, gates, taps, 0, tp_index[0], gated_rows, store)


def mixed_of(arrived, first, count, mix_gain, layer):
    parts = [arrived[t, first : first + count, :].astype(jnp.float32) for t in range(arrived.shape[0])]
    values = jnp.concatenate(parts, axis=1)
    return (values * scale_of(values, values.shape[1]) * mix_gain[layer : layer + 1, :]).astype(jnp.bfloat16)


def project(mixed, out_turned, branch):
    rows = out_turned.shape[0] // PARTS
    for part in range(PARTS):
        here = pl.ds(part * rows, rows)
        product = lax.dot_general(
            mixed, out_turned[here, :], (((1,), (1,)), ((), ())), preferred_element_type=jnp.float32
        )
        branch[:, here] = product.astype(jnp.bfloat16)


def added(stream, branch, post_gain, layer):
    branch = branch.astype(jnp.float32)
    return stream + branch * scale_of(branch, branch.shape[1]) * post_gain[layer : layer + 1, :]


def middle_kernel(
    tp_index, arrived, out_turned, tokens, halo, gates, taps, mix_gain, post_gain, pre_gain,
    raw, residual, mixed, branch, gated_rows,
):
    row_count, width = tokens.shape
    for first, count in in_blocks(row_count):
        mixed[first : first + count, :] = mixed_of(arrived, first, count, mix_gain, 0)
    project(mixed[...], out_turned, branch)
    for first, count in in_blocks(row_count):
        rows = halo[...] if first == 0 else tokens[first - HALO : first - HALO + count, :]
        stream = added(rows.astype(jnp.float32), branch[first : first + count, :], post_gain, 0)
        if first > 0:

            @pl.when(tp_index[0] == (first - HALO) // BLOCK)
            def _():
                residual[...] = stream

        scale = scale_of(stream, width)
        branch[first : first + count, :] = (stream * scale * pre_gain[1:2, :]).astype(jnp.bfloat16)

    def store(values):
        raw[...] = values[HALO:, :]

    mix(branch, gates, taps, 1, tp_index[0], gated_rows, store)


def last_kernel(arrived, out_turned, residual, mix_gain, post_gain, result, branch):
    mixed = mixed_of(arrived, 0, arrived.shape[1], mix_gain, 1)
    project(mixed, out_turned, branch)
    result[...] = added(residual[...], branch[...], post_gain, 1).astype(jnp.bfloat16)


def cost(rows, depth, columns):
    return pl.CostEstimate(flops=2 * rows * depth * columns, bytes_accessed=4 << 20, transcendentals=0)


def per_device(
    tokens, gate_in, gate_conv, value_in, out_weight, conv_taps, pre_gain, mix_gain, post_gain
):
    channels = gate_in.shape[2]
    whole = out_weight.shape[1]
    row_count, width = tokens.shape
    all_rows = HALO + row_count
    tp_size = lax.axis_size("tp")
    sp_size = lax.axis_size("sp")
    tp_index = lax.axis_index("tp")
    share = row_count // tp_size
    params = pltpu.CompilerParams(vmem_limit_bytes=VMEM_LIMIT)
    smem = pl.BlockSpec(memory_space=pltpu.SMEM)
    vmem = pl.BlockSpec(memory_space=pltpu.VMEM)

    packed, tail = pack(tokens, gate_in, gate_conv, value_in, jnp.swapaxes(out_weight, 1, 2))
    halo = lax.ppermute(tail, "sp", [(i, i + 1) for i in range(sp_size - 1)])
    gathered = lax.all_gather(packed.astype(jnp.float16), "sp", axis=0, tiled=True)
    stride = 3 * channels + whole

    def received(start, count, unscale):
        part = gathered[:, start : start + count].astype(jnp.float32) * unscale
        return part.astype(jnp.bfloat16)

    gates = [received(layer * stride, 3 * channels, 1.0 / GATE_SCALE) for layer in range(2)]
    gates, unscale = lax.optimization_barrier((gates, jnp.float32(1.0 / OUT_SCALE)))
    outs = [received(layer * stride + 3 * channels, whole, unscale) for layer in range(2)]
    gates, outs = lax.optimization_barrier((gates, outs))
    tp_index = tp_index.reshape(1)
    raw = pl.pallas_call(
        first_kernel,
        in_specs=[smem] + [vmem] * 5,
        out_specs=vmem,
        out_shape=jax.ShapeDtypeStruct((tp_size, all_rows, channels), jnp.bfloat16),
        scratch_shapes=[
            pltpu.VMEM((all_rows, width), jnp.bfloat16),
            pltpu.VMEM((PAD + all_rows, channels), jnp.float32),
        ],
        compiler_params=params,
        cost_estimate=cost(row_count, width, 3 * channels),
        name="first",
    )(tp_index, tokens, halo, gates[0], conv_taps, pre_gain)
    arrived = lax.all_to_all(raw, "tp", split_axis=0, concat_axis=0, tiled=True)
    raw, residual = pl.pallas_call(
        middle_kernel,
        in_specs=[smem] + [vmem] * 9,
        out_specs=[vmem, vmem],
        out_shape=[
            jax.ShapeDtypeStruct((row_count, channels), jnp.bfloat16),
            jax.ShapeDtypeStruct((share, width), jnp.float32),
        ],
        scratch_shapes=[
            pltpu.VMEM((all_rows, whole), jnp.bfloat16),
            pltpu.VMEM((all_rows, width), jnp.bfloat16),
            pltpu.VMEM((PAD + all_rows, channels), jnp.float32),
        ],
        compiler_params=params,
        cost_estimate=cost(row_count, width, 3 * channels + whole),
        name="middle",
    )(tp_index, arrived, outs[0], tokens, halo, gates[1], conv_taps, mix_gain, post_gain, pre_gain)
    arrived = lax.all_to_all(
        raw.reshape(tp_size, share, channels), "tp", split_axis=0, concat_axis=0, tiled=True
    )
    return pl.pallas_call(
        last_kernel,
        in_specs=[vmem] * 5,
        out_specs=vmem,
        out_shape=jax.ShapeDtypeStruct((share, width), jnp.bfloat16),
        scratch_shapes=[
            pltpu.VMEM((share, width), jnp.bfloat16),
        ],
        compiler_params=params,
        cost_estimate=cost(share, width, whole),
        name="last",
    )(arrived, outs[1], residual, mix_gain, post_gain)


def solution(mesh):
    placed = (
        P(("grp", "sp"), None),
        P(None, "sp", "tp"),
        P(None, "sp", "tp"),
        P(None, "sp", "tp"),
        P(None, None, "sp"),
        P(),
        P(),
        P(),
        P(),
    )
    return jax.shard_map(
        per_device,
        mesh=mesh,
        in_specs=placed,
        out_specs=P(("grp", "sp", "tp"), None),
        check_vma=False,
    )
```

```python
import functools

import jax
import jax.numpy as jnp
from jax import lax
from jax.experimental import pallas as pl
from jax.experimental.pallas import tpu as pltpu
from jax.sharding import PartitionSpec as P

EPS = 1e-06
GATE_SCALE = 2.0**18
OUT_SCALE = 2.0**17
HALO = 16
PAD = 8
BLOCK = 128
VMEM_LIMIT = 16 * 1024 * 1024


def scale_of(values, count):
    return lax.rsqrt(jnp.sum(values * values, axis=-1, keepdims=True) * (1.0 / count) + EPS)


def pack_kernel(gate_in, gate_conv, value_in, out_turned, tail, packed, tail_out):
    layers, _, channels = gate_in.shape
    whole = out_turned.shape[2]
    start = 0
    for layer in range(layers):
        for w in (gate_in, gate_conv, value_in):
            scaled = w[layer].astype(jnp.float32) * GATE_SCALE
            packed[:, start : start + channels] = scaled.astype(jnp.bfloat16)
            start += channels
        scaled = out_turned[layer].astype(jnp.float32) * OUT_SCALE
        packed[:, start : start + whole] = scaled.astype(jnp.bfloat16)
        start += whole
    tail_out[...] = tail[...]


def pack(tokens, gate_in, gate_conv, value_in, out_turned):
    rows = gate_in.shape[1]
    columns = gate_in.shape[0] * (3 * gate_in.shape[2] + out_turned.shape[2])
    count, width = tokens.shape
    return pl.pallas_call(
        pack_kernel,
        grid=(1,),
        in_specs=[
            pl.BlockSpec(gate_in.shape, lambda i: (0, 0, 0)),
            pl.BlockSpec(gate_in.shape, lambda i: (0, 0, 0)),
            pl.BlockSpec(gate_in.shape, lambda i: (0, 0, 0)),
            pl.BlockSpec(out_turned.shape, lambda i: (0, 0, 0)),
            pl.BlockSpec((HALO, width), lambda i: (count // HALO - 1, 0)),
        ],
        out_specs=[
            pl.BlockSpec((rows, columns), lambda i: (0, 0)),
            pl.BlockSpec((HALO, width), lambda i: (0, 0)),
        ],
        out_shape=[
            jax.ShapeDtypeStruct((rows, columns), jnp.bfloat16),
            jax.ShapeDtypeStruct((HALO, width), jnp.bfloat16),
        ],
        name="pack",
    )(gate_in, gate_conv, value_in, out_turned, tokens)


def in_blocks(rows):
    return [(0, HALO)] + [(HALO + start, BLOCK) for start in range(0, rows, BLOCK)]


def normed_kernel(tokens, halo, pre_gain, normed):
    row_count, width = tokens.shape
    for first, count in in_blocks(row_count):
        rows = halo[...] if first == 0 else tokens[first - HALO : first - HALO + count, :]
        stream = rows.astype(jnp.float32)
        scale = scale_of(stream, width)
        normed[first : first + count, :] = (stream * scale * pre_gain[0:1, :]).astype(jnp.bfloat16)


def mix_kernel(layer, spread, tp_index, mixers, taps, raw, gated_rows):
    rows = mixers.shape[0]
    tap_count = taps.shape[1]
    channels = mixers.shape[1] // 3
    mine = pl.ds(pl.multiple_of(tp_index[0] * channels, channels), channels)
    gated = mixers[:, channels : 2 * channels].astype(jnp.float32)
    gated = gated * mixers[:, 2 * channels :].astype(jnp.float32)
    gated_rows[0:PAD, :] = jnp.zeros((PAD, channels), jnp.float32)
    gated_rows[PAD:, :] = gated.astype(jnp.bfloat16).astype(jnp.float32)
    filtered = None
    for tap in range(tap_count):
        at = PAD - (tap_count - 1) + tap
        term = taps[layer, tap : tap + 1, mine] * gated_rows[at : at + rows, :]
        filtered = term if filtered is None else filtered + term
    values = (mixers[:, :channels].astype(jnp.float32) * filtered).astype(jnp.bfloat16)
    if spread:
        for t in range(raw.shape[0]):
            raw[t] = values
    else:
        raw[...] = values[HALO:, :]


def mixed_kernel(layer, arrived, mix_gain, mixed):
    parts = [arrived[t].astype(jnp.float32) for t in range(arrived.shape[0])]
    values = jnp.concatenate(parts, axis=1)
    scale = scale_of(values, values.shape[1])
    mixed[...] = (values * scale * mix_gain[layer : layer + 1, :]).astype(jnp.bfloat16)


def added(stream, branch, post_gain, layer):
    branch = branch.astype(jnp.float32)
    return stream + branch * scale_of(branch, branch.shape[1]) * post_gain[layer : layer + 1, :]


def middle_kernel(tp_index, branch, tokens, halo, post_gain, pre_gain, normed, residual):
    row_count, width = tokens.shape
    for first, count in in_blocks(row_count):
        rows = halo[...] if first == 0 else tokens[first - HALO : first - HALO + count, :]
        stream = added(rows.astype(jnp.float32), branch[first : first + count, :], post_gain, 0)
        if first > 0:

            @pl.when(tp_index[0] == (first - HALO) // BLOCK)
            def _():
                residual[...] = stream

        scale = scale_of(stream, width)
        normed[first : first + count, :] = (stream * scale * pre_gain[1:2, :]).astype(jnp.bfloat16)


def last_kernel(branch, residual, post_gain, result):
    result[...] = added(residual[...], branch[...], post_gain, 1).astype(jnp.bfloat16)


def per_device(
    tokens, gate_in, gate_conv, value_in, out_weight, conv_taps, pre_gain, mix_gain, post_gain
):
    channels = gate_in.shape[2]
    whole = out_weight.shape[1]
    row_count, width = tokens.shape
    all_rows = HALO + row_count
    tp_size = lax.axis_size("tp")
    sp_size = lax.axis_size("sp")
    tp_index = lax.axis_index("tp").reshape(1)
    share = row_count // tp_size
    params = pltpu.CompilerParams(vmem_limit_bytes=VMEM_LIMIT)
    smem = pl.BlockSpec(memory_space=pltpu.SMEM)
    vmem = pl.BlockSpec(memory_space=pltpu.VMEM)

    def call(kernel, name, in_specs, shapes, *operands, scratch=()):
        return pl.pallas_call(
            kernel,
            in_specs=in_specs,
            out_specs=[vmem] * len(shapes),
            out_shape=[jax.ShapeDtypeStruct(shape, dtype) for shape, dtype in shapes],
            scratch_shapes=list(scratch),
            compiler_params=params,
            cost_estimate=pl.CostEstimate(flops=1 << 26, bytes_accessed=4 << 20, transcendentals=0),
            name=name,
        )(*operands)

    packed, tail = pack(tokens, gate_in, gate_conv, value_in, jnp.swapaxes(out_weight, 1, 2))
    halo = lax.ppermute(tail, "sp", [(i, i + 1) for i in range(sp_size - 1)])
    gathered = lax.all_gather(packed.astype(jnp.float16), "sp", axis=0, tiled=True)
    stride = 3 * channels + whole

    def gates(layer):
        part = gathered[:, layer * stride : layer * stride + 3 * channels]
        return (part.astype(jnp.float32) * (1.0 / GATE_SCALE)).astype(jnp.bfloat16)

    def out_turned(layer):
        part = gathered[:, layer * stride + 3 * channels : (layer + 1) * stride]
        return (part.astype(jnp.float32) * (1.0 / OUT_SCALE)).astype(jnp.bfloat16)

    def mixers_of(normed, layer):
        return jnp.dot(normed, gates(layer), preferred_element_type=jnp.float32).astype(jnp.bfloat16)

    def branch_of(mixed, layer):
        product = lax.dot_general(
            mixed, out_turned(layer), (((1,), (1,)), ((), ())), preferred_element_type=jnp.float32
        )
        return product.astype(jnp.bfloat16)

    gated_rows = pltpu.VMEM((PAD + all_rows, channels), jnp.float32)
    bf16, f32 = jnp.bfloat16, jnp.float32
    (normed,) = call(normed_kernel, "normed", [vmem] * 3, [((all_rows, width), bf16)], tokens, halo, pre_gain)
    (raw,) = call(
        functools.partial(mix_kernel, 0, True), "mix0", [smem, vmem, vmem],
        [((tp_size, all_rows, channels), bf16)], tp_index, mixers_of(normed, 0), conv_taps, scratch=(gated_rows,),
    )
    arrived = lax.all_to_all(raw, "tp", split_axis=0, concat_axis=0, tiled=True)
    (mixed,) = call(
        functools.partial(mixed_kernel, 0), "mixed0", [vmem] * 2, [((all_rows, whole), bf16)], arrived, mix_gain
    )
    normed, residual = call(
        middle_kernel, "middle", [smem] + [vmem] * 5, [((all_rows, width), bf16), ((share, width), f32)],
        tp_index, branch_of(mixed, 0), tokens, halo, post_gain, pre_gain,
    )
    (raw,) = call(
        functools.partial(mix_kernel, 1, False), "mix1", [smem, vmem, vmem],
        [((row_count, channels), bf16)], tp_index, mixers_of(normed, 1), conv_taps, scratch=(gated_rows,),
    )
    arrived = lax.all_to_all(
        raw.reshape(tp_size, share, channels), "tp", split_axis=0, concat_axis=0, tiled=True
    )
    (mixed,) = call(
        functools.partial(mixed_kernel, 1), "mixed1", [vmem] * 2, [((share, whole), bf16)], arrived, mix_gain
    )
    (result,) = call(
        last_kernel, "last", [vmem] * 3, [((share, width), bf16)], branch_of(mixed, 1), residual, post_gain
    )
    return result


def solution(mesh):
    placed = (
        P(("grp", "sp"), None),
        P(None, "sp", "tp"),
        P(None, "sp", "tp"),
        P(None, "sp", "tp"),
        P(None, None, "sp"),
        P(),
        P(),
        P(),
        P(),
    )
    return jax.shard_map(
        per_device,
        mesh=mesh,
        in_specs=placed,
        out_specs=P(("grp", "sp", "tp"), None),
        check_vma=False,
    )
```

```python
import functools

import jax
import jax.numpy as jnp
from jax import lax
from jax.experimental import pallas as pl
from jax.experimental.pallas import tpu as pltpu
from jax.sharding import PartitionSpec as P

EPS = 1e-06
GATE_SCALE = 2.0**18
OUT_SCALE = 2.0**17
HALO = 16
PAD = 8
BLOCK = 128
VMEM_LIMIT = 16 * 1024 * 1024


def scale_of(values, count):
    return lax.rsqrt(jnp.sum(values * values, axis=-1, keepdims=True) * (1.0 / count) + EPS)


def tail_kernel(tail, tail_out):
    tail_out[...] = tail[...]


def tail_of(tokens):
    count, width = tokens.shape
    return pl.pallas_call(
        tail_kernel,
        grid=(1,),
        in_specs=[pl.BlockSpec((HALO, width), lambda i: (count // HALO - 1, 0))],
        out_specs=pl.BlockSpec((HALO, width), lambda i: (0, 0)),
        out_shape=jax.ShapeDtypeStruct((HALO, width), jnp.bfloat16),
        name="tail",
    )(tokens)


def pack_kernel(gate_in, gate_conv, value_in, out_turned, packed):
    layers, _, channels = gate_in.shape
    whole = out_turned.shape[2]
    start = 0
    for layer in range(layers):
        for w in (gate_in, gate_conv, value_in):
            scaled = w[layer].astype(jnp.float32) * GATE_SCALE
            packed[:, start : start + channels] = scaled.astype(jnp.bfloat16)
            start += channels
        scaled = out_turned[layer].astype(jnp.float32) * OUT_SCALE
        packed[:, start : start + whole] = scaled.astype(jnp.bfloat16)
        start += whole


def pack(gate_in, gate_conv, value_in, out_turned):
    rows = gate_in.shape[1]
    columns = gate_in.shape[0] * (3 * gate_in.shape[2] + out_turned.shape[2])
    return pl.pallas_call(
        pack_kernel,
        grid=(1,),
        in_specs=[
            pl.BlockSpec(gate_in.shape, lambda i: (0, 0, 0)),
            pl.BlockSpec(gate_in.shape, lambda i: (0, 0, 0)),
            pl.BlockSpec(gate_in.shape, lambda i: (0, 0, 0)),
            pl.BlockSpec(out_turned.shape, lambda i: (0, 0, 0)),
        ],
        out_specs=pl.BlockSpec((rows, columns), lambda i: (0, 0)),
        out_shape=jax.ShapeDtypeStruct((rows, columns), jnp.bfloat16),
        name="pack",
    )(gate_in, gate_conv, value_in, out_turned)


def in_blocks(rows):
    return [(0, HALO)] + [(HALO + start, BLOCK) for start in range(0, rows, BLOCK)]


def normed_kernel(tokens, halo, pre_gain, normed):
    row_count, width = tokens.shape
    for first, count in in_blocks(row_count):
        rows = halo[...] if first == 0 else tokens[first - HALO : first - HALO + count, :]
        stream = rows.astype(jnp.float32)
        scale = scale_of(stream, width)
        normed[first : first + count, :] = (stream * scale * pre_gain[0:1, :]).astype(jnp.bfloat16)


def mix_kernel(layer, spread, tp_index, mixers, taps, raw, gated_rows):
    rows = mixers.shape[0]
    tap_count = taps.shape[1]
    channels = mixers.shape[1] // 3
    mine = pl.ds(pl.multiple_of(tp_index[0] * channels, channels), channels)
    gated = mixers[:, channels : 2 * channels].astype(jnp.float32)
    gated = gated * mixers[:, 2 * channels :].astype(jnp.float32)
    gated_rows[0:PAD, :] = jnp.zeros((PAD, channels), jnp.float32)
    gated_rows[PAD:, :] = gated.astype(jnp.bfloat16).astype(jnp.float32)
    filtered = None
    for tap in range(tap_count):
        at = PAD - (tap_count - 1) + tap
        term = taps[layer, tap : tap + 1, mine] * gated_rows[at : at + rows, :]
        filtered = term if filtered is None else filtered + term
    values = (mixers[:, :channels].astype(jnp.float32) * filtered).astype(jnp.bfloat16)
    if spread:
        for t in range(raw.shape[0]):
            raw[t] = values
    else:
        raw[...] = values[HALO:, :]


def mixed_kernel(layer, arrived, mix_gain, mixed):
    parts = [arrived[t].astype(jnp.float32) for t in range(arrived.shape[0])]
    values = jnp.concatenate(parts, axis=1)
    scale = scale_of(values, values.shape[1])
    mixed[...] = (values * scale * mix_gain[layer : layer + 1, :]).astype(jnp.bfloat16)


def added(stream, branch, post_gain, layer):
    branch = branch.astype(jnp.float32)
    return stream + branch * scale_of(branch, branch.shape[1]) * post_gain[layer : layer + 1, :]


def middle_kernel(tp_index, branch, tokens, halo, post_gain, pre_gain, normed, residual):
    row_count, width = tokens.shape
    for first, count in in_blocks(row_count):
        rows = halo[...] if first == 0 else tokens[first - HALO : first - HALO + count, :]
        stream = added(rows.astype(jnp.float32), branch[first : first + count, :], post_gain, 0)
        if first > 0:

            @pl.when(tp_index[0] == (first - HALO) // BLOCK)
            def _():
                residual[...] = stream

        scale = scale_of(stream, width)
        normed[first : first + count, :] = (stream * scale * pre_gain[1:2, :]).astype(jnp.bfloat16)


def last_kernel(branch, residual, post_gain, result):
    result[...] = added(residual[...], branch[...], post_gain, 1).astype(jnp.bfloat16)


def per_device(
    tokens, gate_in, gate_conv, value_in, out_weight, conv_taps, pre_gain, mix_gain, post_gain
):
    channels = gate_in.shape[2]
    whole = out_weight.shape[1]
    row_count, width = tokens.shape
    all_rows = HALO + row_count
    tp_size = lax.axis_size("tp")
    sp_size = lax.axis_size("sp")
    tp_index = lax.axis_index("tp").reshape(1)
    share = row_count // tp_size
    params = pltpu.CompilerParams(vmem_limit_bytes=VMEM_LIMIT)
    smem = pl.BlockSpec(memory_space=pltpu.SMEM)
    vmem = pl.BlockSpec(memory_space=pltpu.VMEM)

    def call(kernel, name, in_specs, shapes, *operands, scratch=()):
        return pl.pallas_call(
            kernel,
            in_specs=in_specs,
            out_specs=[vmem] * len(shapes),
            out_shape=[jax.ShapeDtypeStruct(shape, dtype) for shape, dtype in shapes],
            scratch_shapes=list(scratch),
            compiler_params=params,
            cost_estimate=pl.CostEstimate(flops=1 << 26, bytes_accessed=4 << 20, transcendentals=0),
            name=name,
        )(*operands)

    packed = pack(gate_in, gate_conv, value_in, jnp.swapaxes(out_weight, 1, 2))
    halo = lax.ppermute(tail_of(tokens), "sp", [(i, i + 1) for i in range(sp_size - 1)])
    bf16, f32 = jnp.bfloat16, jnp.float32
    (normed,) = call(normed_kernel, "normed", [vmem] * 3, [((all_rows, width), bf16)], tokens, halo, pre_gain)
    sent, normed = lax.optimization_barrier((packed.astype(jnp.float16), normed))
    gathered = lax.all_gather(sent, "sp", axis=0, tiled=True)
    stride = 3 * channels + whole

    def gates(layer):
        part = gathered[:, layer * stride : layer * stride + 3 * channels]
        return (part.astype(jnp.float32) * (1.0 / GATE_SCALE)).astype(jnp.bfloat16)

    def out_turned(layer):
        part = gathered[:, layer * stride + 3 * channels : (layer + 1) * stride]
        return (part.astype(jnp.float32) * (1.0 / OUT_SCALE)).astype(jnp.bfloat16)

    def mixers_of(normed, layer):
        return jnp.dot(normed, gates(layer), preferred_element_type=jnp.float32).astype(jnp.bfloat16)

    def branch_of(mixed, layer):
        product = lax.dot_general(
            mixed, out_turned(layer), (((1,), (1,)), ((), ())), preferred_element_type=jnp.float32
        )
        return product.astype(jnp.bfloat16)

    gated_rows = pltpu.VMEM((PAD + all_rows, channels), jnp.float32)
    (raw,) = call(
        functools.partial(mix_kernel, 0, True), "mix0", [smem, vmem, vmem],
        [((tp_size, all_rows, channels), bf16)], tp_index, mixers_of(normed, 0), conv_taps, scratch=(gated_rows,),
    )
    arrived = lax.all_to_all(raw, "tp", split_axis=0, concat_axis=0, tiled=True)
    (mixed,) = call(
        functools.partial(mixed_kernel, 0), "mixed0", [vmem] * 2, [((all_rows, whole), bf16)], arrived, mix_gain
    )
    normed, residual = call(
        middle_kernel, "middle", [smem] + [vmem] * 5, [((all_rows, width), bf16), ((share, width), f32)],
        tp_index, branch_of(mixed, 0), tokens, halo, post_gain, pre_gain,
    )
    (raw,) = call(
        functools.partial(mix_kernel, 1, False), "mix1", [smem, vmem, vmem],
        [((row_count, channels), bf16)], tp_index, mixers_of(normed, 1), conv_taps, scratch=(gated_rows,),
    )
    arrived = lax.all_to_all(
        raw.reshape(tp_size, share, channels), "tp", split_axis=0, concat_axis=0, tiled=True
    )
    (mixed,) = call(
        functools.partial(mixed_kernel, 1), "mixed1", [vmem] * 2, [((share, whole), bf16)], arrived, mix_gain
    )
    (result,) = call(
        last_kernel, "last", [vmem] * 3, [((share, width), bf16)], branch_of(mixed, 1), residual, post_gain
    )
    return result


def solution(mesh):
    placed = (
        P(("grp", "sp"), None),
        P(None, "sp", "tp"),
        P(None, "sp", "tp"),
        P(None, "sp", "tp"),
        P(None, None, "sp"),
        P(),
        P(),
        P(),
        P(),
    )
    return jax.shard_map(
        per_device,
        mesh=mesh,
        in_specs=placed,
        out_specs=P(("grp", "sp", "tp"), None),
        check_vma=False,
    )
```

```python
import functools

import jax
import jax.numpy as jnp
from jax import lax
from jax.experimental import pallas as pl
from jax.experimental.pallas import tpu as pltpu
from jax.sharding import PartitionSpec as P

EPS = 1e-06
GATE_SCALE = 2.0**18
OUT_SCALE = 2.0**17
HALO = 8
PAD = 8
BLOCK = 128
VMEM_LIMIT = 16 * 1024 * 1024


def scale_of(values, count):
    return lax.rsqrt(jnp.sum(values * values, axis=-1, keepdims=True) * (1.0 / count) + EPS)


def tail_kernel(tail, tail_out):
    tail_out[...] = tail[...]


def tail_of(tokens):
    count, width = tokens.shape
    return pl.pallas_call(
        tail_kernel,
        grid=(1,),
        in_specs=[pl.BlockSpec((HALO, width), lambda i: (count // HALO - 1, 0))],
        out_specs=pl.BlockSpec((HALO, width), lambda i: (0, 0)),
        out_shape=jax.ShapeDtypeStruct((HALO, width), jnp.bfloat16),
        name="tail",
    )(tokens)


def pack_kernel(gate_in, gate_conv, value_in, out_turned, packed):
    layers, _, channels = gate_in.shape
    whole = out_turned.shape[2]
    start = 0
    for layer in range(layers):
        for w in (gate_in, gate_conv, value_in):
            scaled = w[layer].astype(jnp.float32) * GATE_SCALE
            packed[:, start : start + channels] = scaled.astype(jnp.bfloat16)
            start += channels
        scaled = out_turned[layer].astype(jnp.float32) * OUT_SCALE
        packed[:, start : start + whole] = scaled.astype(jnp.bfloat16)
        start += whole


def pack(gate_in, gate_conv, value_in, out_turned):
    rows = gate_in.shape[1]
    columns = gate_in.shape[0] * (3 * gate_in.shape[2] + out_turned.shape[2])
    return pl.pallas_call(
        pack_kernel,
        grid=(1,),
        in_specs=[
            pl.BlockSpec(gate_in.shape, lambda i: (0, 0, 0)),
            pl.BlockSpec(gate_in.shape, lambda i: (0, 0, 0)),
            pl.BlockSpec(gate_in.shape, lambda i: (0, 0, 0)),
            pl.BlockSpec(out_turned.shape, lambda i: (0, 0, 0)),
        ],
        out_specs=pl.BlockSpec((rows, columns), lambda i: (0, 0)),
        out_shape=jax.ShapeDtypeStruct((rows, columns), jnp.bfloat16),
        name="pack",
    )(gate_in, gate_conv, value_in, out_turned)


def in_blocks(rows):
    return [(0, HALO)] + [(HALO + start, BLOCK) for start in range(0, rows, BLOCK)]


def normed_kernel(tokens, halo, pre_gain, normed):
    row_count, width = tokens.shape
    for first, count in in_blocks(row_count):
        rows = halo[...] if first == 0 else tokens[first - HALO : first - HALO + count, :]
        stream = rows.astype(jnp.float32)
        scale = scale_of(stream, width)
        normed[first : first + count, :] = (stream * scale * pre_gain[0:1, :]).astype(jnp.bfloat16)


def mix_kernel(layer, spread, tp_index, mixers, taps, raw, gated_rows):
    rows = mixers.shape[0]
    tap_count = taps.shape[1]
    channels = mixers.shape[1] // 3
    mine = pl.ds(pl.multiple_of(tp_index[0] * channels, channels), channels)
    gated = mixers[:, channels : 2 * channels].astype(jnp.float32)
    gated = gated * mixers[:, 2 * channels :].astype(jnp.float32)
    gated_rows[0:PAD, :] = jnp.zeros((PAD, channels), jnp.float32)
    gated_rows[PAD:, :] = gated.astype(jnp.bfloat16).astype(jnp.float32)
    filtered = None
    for tap in range(tap_count):
        at = PAD - (tap_count - 1) + tap
        term = taps[layer, tap : tap + 1, mine] * gated_rows[at : at + rows, :]
        filtered = term if filtered is None else filtered + term
    values = (mixers[:, :channels].astype(jnp.float32) * filtered).astype(jnp.bfloat16)
    if spread:
        for t in range(raw.shape[0]):
            raw[t] = values
    else:
        raw[...] = values[HALO:, :]


def mixed_kernel(layer, arrived, mix_gain, mixed):
    parts = [arrived[t].astype(jnp.float32) for t in range(arrived.shape[0])]
    values = jnp.concatenate(parts, axis=1)
    scale = scale_of(values, values.shape[1])
    mixed[...] = (values * scale * mix_gain[layer : layer + 1, :]).astype(jnp.bfloat16)


def added(stream, branch, post_gain, layer):
    branch = branch.astype(jnp.float32)
    return stream + branch * scale_of(branch, branch.shape[1]) * post_gain[layer : layer + 1, :]


def middle_kernel(tp_index, branch, tokens, halo, post_gain, pre_gain, normed, residual):
    row_count, width = tokens.shape
    for first, count in in_blocks(row_count):
        rows = halo[...] if first == 0 else tokens[first - HALO : first - HALO + count, :]
        stream = added(rows.astype(jnp.float32), branch[first : first + count, :], post_gain, 0)
        if first > 0:

            @pl.when(tp_index[0] == (first - HALO) // BLOCK)
            def _():
                residual[...] = stream

        scale = scale_of(stream, width)
        normed[first : first + count, :] = (stream * scale * pre_gain[1:2, :]).astype(jnp.bfloat16)


def last_kernel(branch, residual, post_gain, result):
    result[...] = added(residual[...], branch[...], post_gain, 1).astype(jnp.bfloat16)


def per_device(
    tokens, gate_in, gate_conv, value_in, out_weight, conv_taps, pre_gain, mix_gain, post_gain
):
    channels = gate_in.shape[2]
    whole = out_weight.shape[1]
    row_count, width = tokens.shape
    all_rows = HALO + row_count
    tp_size = lax.axis_size("tp")
    sp_size = lax.axis_size("sp")
    tp_index = lax.axis_index("tp").reshape(1)
    share = row_count // tp_size
    params = pltpu.CompilerParams(vmem_limit_bytes=VMEM_LIMIT)
    smem = pl.BlockSpec(memory_space=pltpu.SMEM)
    vmem = pl.BlockSpec(memory_space=pltpu.VMEM)

    def call(kernel, name, in_specs, shapes, *operands, scratch=()):
        return pl.pallas_call(
            kernel,
            in_specs=in_specs,
            out_specs=[vmem] * len(shapes),
            out_shape=[jax.ShapeDtypeStruct(shape, dtype) for shape, dtype in shapes],
            scratch_shapes=list(scratch),
            compiler_params=params,
            cost_estimate=pl.CostEstimate(flops=1 << 26, bytes_accessed=4 << 20, transcendentals=0),
            name=name,
        )(*operands)

    packed = pack(gate_in, gate_conv, value_in, jnp.swapaxes(out_weight, 1, 2))
    halo = lax.ppermute(tail_of(tokens), "sp", [(i, i + 1) for i in range(sp_size - 1)])
    bf16, f32 = jnp.bfloat16, jnp.float32
    (normed,) = call(normed_kernel, "normed", [vmem] * 3, [((all_rows, width), bf16)], tokens, halo, pre_gain)
    sent, normed = lax.optimization_barrier((packed.astype(jnp.float16), normed))
    gathered = lax.all_gather(sent, "sp", axis=0, tiled=True)
    stride = 3 * channels + whole

    def gates(layer):
        part = gathered[:, layer * stride : layer * stride + 3 * channels]
        return (part.astype(jnp.float32) * (1.0 / GATE_SCALE)).astype(jnp.bfloat16)

    def out_turned(layer):
        part = gathered[:, layer * stride + 3 * channels : (layer + 1) * stride]
        return (part.astype(jnp.float32) * (1.0 / OUT_SCALE)).astype(jnp.bfloat16)

    def mixers_of(normed, layer):
        return jnp.dot(normed, gates(layer), preferred_element_type=jnp.float32).astype(jnp.bfloat16)

    def branch_of(mixed, layer):
        product = lax.dot_general(
            mixed, out_turned(layer), (((1,), (1,)), ((), ())), preferred_element_type=jnp.float32
        )
        return product.astype(jnp.bfloat16)

    gated_rows = pltpu.VMEM((PAD + all_rows, channels), jnp.float32)
    (raw,) = call(
        functools.partial(mix_kernel, 0, True), "mix0", [smem, vmem, vmem],
        [((tp_size, all_rows, channels), bf16)], tp_index, mixers_of(normed, 0), conv_taps, scratch=(gated_rows,),
    )
    arrived = lax.all_to_all(raw, "tp", split_axis=0, concat_axis=0, tiled=True)
    (mixed,) = call(
        functools.partial(mixed_kernel, 0), "mixed0", [vmem] * 2, [((all_rows, whole), bf16)], arrived, mix_gain
    )
    normed, residual = call(
        middle_kernel, "middle", [smem] + [vmem] * 5, [((all_rows, width), bf16), ((share, width), f32)],
        tp_index, branch_of(mixed, 0), tokens, halo, post_gain, pre_gain,
    )
    (raw,) = call(
        functools.partial(mix_kernel, 1, False), "mix1", [smem, vmem, vmem],
        [((row_count, channels), bf16)], tp_index, mixers_of(normed, 1), conv_taps, scratch=(gated_rows,),
    )
    arrived = lax.all_to_all(
        raw.reshape(tp_size, share, channels), "tp", split_axis=0, concat_axis=0, tiled=True
    )
    (mixed,) = call(
        functools.partial(mixed_kernel, 1), "mixed1", [vmem] * 2, [((share, whole), bf16)], arrived, mix_gain
    )
    (result,) = call(
        last_kernel, "last", [vmem] * 3, [((share, width), bf16)], branch_of(mixed, 1), residual, post_gain
    )
    return result


def solution(mesh):
    placed = (
        P(("grp", "sp"), None),
        P(None, "sp", "tp"),
        P(None, "sp", "tp"),
        P(None, "sp", "tp"),
        P(None, None, "sp"),
        P(),
        P(),
        P(),
        P(),
    )
    return jax.shard_map(
        per_device,
        mesh=mesh,
        in_specs=placed,
        out_specs=P(("grp", "sp", "tp"), None),
        check_vma=False,
    )
```
